32 devices in a mesh: fs: 4 (over y, x), tp: 8 (over z, core).
Axes of the slice: x: 2, y: 2, z: 4, core: 2. Of those that a mesh axis runs over, the one named last changes fastest.
Arguments:
- tokens: bfloat16 [1024, 2048], P('fs', 'tp'), may hold values from -60 to 60
- norm_gain: float32 [2048], P('fs'), may hold values from 0.1 to 1.9
- gate_weight: float32 [4, 2048, 4096], P(None, 'fs', 'tp'), may hold values from -0.125 to 0.125
- up_weight: float32 [4, 2048, 4096], P(None, 'fs', 'tp'), may hold values from -0.125 to 0.125
- down_weight: float32 [4, 2048, 4096], P(None, 'fs', 'tp'), may hold values from -0.125 to 0.125
- route: int32 [1024, 2], P('fs'), may hold values from 0 to 3, all different within a row; in each aligned block of 256 rows (0 to 255, 256 to 511, ...) at most 256 rows name the same one
- route_weight: float32 [1024, 2], P('fs'), may hold values from 0.2 to 1
Outputs:
- mixed: bfloat16 [1024, 2048], P('fs', 'tp')
- gate_new: bfloat16 [4, 2048, 4096], P('fs', None, 'tp')
- up_new: bfloat16 [4, 2048, 4096], P('fs', None, 'tp')
- down_new: bfloat16 [4, 2048, 4096], P('fs', None, 'tp')
The draws below stay inside these ranges and needn't reach their ends.
Inputs may be any that keep to these rules, and one draw needn't show every extreme that they name: `route`: the 2 experts of a row differ. In each aligned block of 256 rows (the tokens of one index of fs) no expert is named by more than 256 rows, a bound that some block reaches.
All inputs are finite; a program needn't handle non-finite values.
Results may differ from the reference program's by a relative error of at most 0.024.
Values may be sent and summed in bfloat16 or wider, within the bound.
A program may use at most 64 MiB of HBM per device.

```python
import math
import jax
import jax.numpy as jnp
import numpy as np
from jax import lax

D = 2048
FF = 4096
TOP = 2
TOK_DEV = 256
EXPERTS = 4
CAP = 256
TOKENS = 1024
N_FS = 4
N_TP = 8


def draw_tokens(key, part):
    key_base = jax.random.fold_in(key, 11)
    values = jax.random.normal(key_base, (TOKENS, D), jnp.float32)
    column_scale = 0.6 * 3.0 ** (jnp.arange(D, dtype=jnp.float32) / D)
    values = jnp.clip(values * column_scale[None, :], -60.0, 60.0)
    return values.astype(jnp.bfloat16)


def strengthened(result, own_key, source, target, parts, factor):
    def block_of(dim):
        return (jnp.arange(result.shape[dim]) // (result.shape[dim] // parts)).reshape((-1,) + (1,) * (result.ndim - 1 - dim))

    first = jax.random.permutation(own_key, parts)[block_of(target)]
    other_side = (block_of(target) + parts // 2) % parts
    return jnp.where((block_of(source) == first) | (block_of(source) == other_side), factor * result, result)


def block_levels(rng, extent, cuts, least, top_value):
    gain = 1.0
    for dim, blocks in cuts:
        heights = jax.random.uniform(jax.random.fold_in(jax.random.fold_in(rng, 6), dim), (blocks,), jnp.float32, least / len(cuts), top_value / len(cuts))
        gain = gain * jnp.repeat(jnp.exp(heights), extent[dim] // blocks).reshape((-1,) + (1,) * (len(extent) - 1 - dim))
    return gain


def assign_block(stream_key, own, number, rows, amount, top, bound, slope):
    ranking = jax.random.permutation(stream_key, amount)
    heavy_load, ordinary = portions_of(amount, rows * top, bound, slope, True), portions_of(amount, rows * top, bound, slope, False)
    places = jnp.arange(amount)

    def named(tallies, offset_by):
        used = int((tallies > 0).sum())
        fixed = max(1, used // 4)
        moved = fixed + (places - fixed + offset_by * (used - fixed)) % max(1, amount - fixed)
        return jnp.zeros((amount,), jnp.int32).at[ranking[jnp.where(places < fixed, places, moved)]].set(jnp.asarray(tallies, jnp.int32))

    tallies = jnp.where(number % 4 == 0, named(heavy_load, number // 4), named(ordinary, number - number // 4 - 1))
    mixed = jax.random.permutation(jax.random.fold_in(own, 3), amount)
    donor, receiver = mixed[0:amount // 2 * 2:2], mixed[1:amount // 2 * 2:2]
    slack = jnp.minimum(tallies[donor] - 1, bound - tallies[receiver]) // 2
    slack = jnp.where((donor == ranking[0]) | (receiver == ranking[0]) | (tallies[receiver] == 0), 0, jnp.maximum(slack, 0))
    moved = jax.random.randint(jax.random.fold_in(own, 4), (amount // 2,), 0, 1 << 20) % (slack + 1)
    tallies = tallies.at[donor].add(-moved).at[receiver].add(moved)
    members = jnp.searchsorted(jnp.cumsum(tallies), jnp.arange(rows * top), side="right").astype(jnp.int32)
    table = members.reshape(top, rows).T
    table = table[jax.random.permutation(jax.random.fold_in(own, 1), rows)]
    offset_by = jax.random.randint(jax.random.fold_in(own, 2), (rows, 1), 0, top)
    return jnp.take_along_axis(table, (jnp.arange(top)[None, :] + offset_by) % top, axis=1)


def portions_of(amount, total, reach, skew, full):
    weights = [(1 << 20) // math.isqrt(grade ** skew) + 1 for grade in range(1, amount + 1)]
    largest = reach if full else min(reach, max(-(-total // amount), total * weights[0] // sum(weights)))
    least = 1 if total - largest >= amount - 1 else 0
    given, spare = [largest] + [least] * (amount - 1), total - largest - least * (amount - 1)
    while spare > 0:
        candidates = [i for i in range(1, amount) if given[i] < largest] or [i for i in range(1, amount) if given[i] < reach]
        pool, remaining = sum([weights[i] for i in candidates]), spare
        for i in candidates:
            more = min(reach - given[i], max(1, remaining * weights[i] // pool), spare)
            given[i] = given[i] + more
            spare = spare - more
    return np.array(given)


def noise(rng, dims, spread, bound, pieces=(), kind=jnp.bfloat16):
    factor_of = block_levels(rng, dims, pieces, -0.22, 0.18) if pieces else 1.0
    entries = jax.random.normal(rng, dims, jnp.float32) * spread * factor_of
    return jnp.minimum(jnp.maximum(entries, -bound), bound).astype(kind)


def gaussian_with(stream_key, extent, spread, most, split, heavy, kind=jnp.bfloat16):
    drawn = spread * jax.random.normal(stream_key, extent, jnp.float32)
    if split:
        drawn = drawn * block_levels(stream_key, extent, split, -0.22, 0.18)
    return jnp.clip(strengthened(drawn, jax.random.fold_in(stream_key, 3), *heavy), -most, most).astype(kind)


def setup_inputs(seed: int = 0) -> dict:
    streams_of = jax.random.split(jax.random.key(seed), 8)
    tokens = draw_tokens(jax.random.fold_in(streams_of[7], 71), 0)
    norm_gain = jnp.clip(1.0 + 0.18 * jax.random.normal(streams_of[1], (D,), jnp.float32), 0.1, 1.9)
    gate_weight = noise(streams_of[2], (EXPERTS, D, FF), D ** -0.5, 0.125, ((1, 4), (2, 8)), jnp.float32)
    up_weight = noise(streams_of[3], (EXPERTS, D, FF), D ** -0.5, 0.125, ((1, 4), (2, 8)), jnp.float32)
    down_weight = gaussian_with(streams_of[4], (EXPERTS, D, FF), FF ** -0.5, 0.125, ((1, 4), (2, 8)), (2, 1, 8, 2.0), jnp.float32)
    route_keys = jax.random.split(jax.random.fold_in(streams_of[5], 1), TOKENS // TOK_DEV)
    route_turns = jax.random.permutation(jax.random.fold_in(streams_of[5], 3), TOKENS // TOK_DEV)
    route = jax.vmap(lambda own, number: assign_block(jax.random.fold_in(streams_of[5], 2), own, number, TOK_DEV, EXPERTS, TOP, CAP, 2))(route_keys, route_turns).reshape((TOKENS, TOP))
    route_weight = jnp.clip(jnp.exp(math.log(1.0) - 1.609438 * jax.random.uniform(streams_of[6], (TOKENS, TOP), jnp.float32) ** block_levels(streams_of[6], (TOKENS, TOP), ((0, 4),), -0.2, 0.2)), 0.2, 1.0)
    return {"tokens": tokens, "norm_gain": norm_gain, "gate_weight": gate_weight, "up_weight": up_weight, "down_weight": down_weight, "route": route, "route_weight": route_weight}


epsilon = 1e-05

def slot_table(route, block_rows, expert_count):
    pair_ids = route.reshape(-1, block_rows * route.shape[1])
    onehot = (pair_ids[:, :, None] == jnp.arange(expert_count, dtype=jnp.int32)[None, None, :]).astype(jnp.int32)
    before = jnp.cumsum(onehot, axis=1) - onehot
    return lax.optimization_barrier(jnp.sum(before * onehot, axis=2)).astype(jnp.int32).reshape(route.shape)

def reference(tokens, norm_gain, gate_weight, up_weight, down_weight, route, route_weight):
    gain_col = norm_gain.astype(jnp.float32)[None, :, None]
    gate_new = (gate_weight * gain_col).astype(jnp.bfloat16)
    up_new = (up_weight * gain_col).astype(jnp.bfloat16)
    down_new = down_weight.astype(jnp.bfloat16)
    tok_float = tokens.astype(jnp.float32)
    normed = (tok_float * lax.rsqrt(lax.optimization_barrier(jnp.mean(tok_float * tok_float, axis=1, keepdims=True)) + epsilon)).astype(jnp.bfloat16)
    slot_of = slot_table(route, TOK_DEV, EXPERTS)
    groups = jnp.broadcast_to((jnp.arange(TOKENS, dtype=jnp.int32) // TOK_DEV)[:, None], route.shape)
    token_index = jnp.broadcast_to(jnp.arange(TOKENS, dtype=jnp.int32)[:, None], route.shape)
    row_table = jnp.full((EXPERTS, N_FS, CAP), TOKENS, jnp.int32).at[route, groups, slot_of].set(token_index)
    padded = jnp.concatenate([normed, jnp.zeros((1, D), jnp.bfloat16)], axis=0)
    block_width = FF // N_TP

    def one_expert(operands):
        gate_e, up_e, down_e, rows_e = operands
        expert_rows = padded[rows_e.reshape(-1)]
        gate_acc = jnp.dot(expert_rows, gate_e, preferred_element_type=jnp.float32)
        up_acc = jnp.dot(expert_rows, up_e, preferred_element_type=jnp.float32)
        hidden = (jax.nn.silu(gate_acc) * up_acc).astype(jnp.bfloat16)

        def add_block(block, running):
            offset = jnp.asarray(block, jnp.int32) * block_width
            part_hidden = lax.dynamic_slice_in_dim(hidden, offset, block_width, 1)
            part_weight = lax.dynamic_slice_in_dim(down_e, offset, block_width, 1)
            term = lax.dot_general(part_hidden, part_weight, (((1,), (1,)), ((), ())), preferred_element_type=jnp.float32)
            return running + term.astype(jnp.bfloat16).astype(jnp.float32)
        summed = lax.fori_loop(0, N_TP, add_block, jnp.zeros((N_FS * CAP, D), jnp.float32))
        return summed.astype(jnp.bfloat16)
    outputs = lax.map(one_expert, (gate_new, up_new, down_new, row_table))
    flat = outputs.reshape(EXPERTS * N_FS * CAP, D)
    index = ((route * N_FS + groups) * CAP + slot_of).astype(jnp.int32)
    picked = flat[index].astype(jnp.float32)
    mixed = lax.optimization_barrier(jnp.sum(picked * route_weight.astype(jnp.float32)[:, :, None], axis=1)).astype(jnp.bfloat16)
    return (mixed, gate_new, up_new, down_new)
```

```python
import functools

import jax
import jax.numpy as jnp
from jax import lax
from jax.experimental import pallas as pl
from jax.experimental.pallas import tpu as pltpu
from jax.sharding import PartitionSpec as P

epsilon = 1e-05


def slot_table(route, block_rows, expert_count):
    pair_ids = route.reshape(-1, block_rows * route.shape[1])
    onehot = (
        pair_ids[:, :, None] == jnp.arange(expert_count, dtype=jnp.int32)[None, None, :]
    ).astype(jnp.int32)
    before = jnp.cumsum(onehot, axis=1) - onehot
    return jnp.sum(before * onehot, axis=2).reshape(route.shape)


def slotted_body(tokens, norm_gain, gate_weight, up_weight, down_weight, route, route_weight):
    experts = gate_weight.shape[0]
    tok_rows = tokens.shape[0]
    columns = tokens.shape[1]
    fs_count = lax.axis_size("fs")
    capacity = 4 * tok_rows // fs_count
    gain_col = norm_gain[None, :, None]
    gate_cast = (gate_weight * gain_col).astype(jnp.bfloat16)
    up_cast = (up_weight * gain_col).astype(jnp.bfloat16)
    down_cast = down_weight.astype(jnp.bfloat16)
    gate_new, up_new, down_new = (
        lax.all_to_all(gate_cast, "fs", split_axis=0, concat_axis=1, tiled=True),
        lax.all_to_all(up_cast, "fs", split_axis=0, concat_axis=1, tiled=True),
        lax.all_to_all(down_cast, "fs", split_axis=0, concat_axis=1, tiled=True),
    )
    slot_of = slot_table(route, tok_rows, experts)
    target = route * capacity + slot_of
    slot_lanes = jnp.arange(experts * capacity, dtype=jnp.int32)
    slot_hits = target[:, :, None] == slot_lanes[None, None, :]
    token_iota = jnp.arange(tok_rows, dtype=jnp.int32)[:, None, None]
    lane_token = jnp.sum(jnp.where(slot_hits, token_iota + 1, 0), axis=(0, 1)) - 1
    lane_token = jnp.where(lane_token < 0, tok_rows, lane_token)
    combine = jnp.sum(jnp.where(slot_hits, route_weight[:, :, None], 0.0), axis=1)
    tok_float = tokens.astype(jnp.float32)
    square_sum = lax.psum(jnp.sum(tok_float * tok_float, axis=1), "tp")
    full_width = columns * lax.axis_size("tp")
    normed = (tok_float * lax.rsqrt(square_sum / full_width + epsilon)[:, None]).astype(
        jnp.bfloat16
    )
    padded = jnp.concatenate([normed, jnp.zeros((1, columns), jnp.bfloat16)], axis=0)
    outgoing = padded[lane_token].reshape(experts, capacity, columns)
    arrived = lax.all_to_all(outgoing, "fs", split_axis=0, concat_axis=0, tiled=True).reshape(
        -1, columns
    )
    gate_local = gate_new[0]
    up_local = up_new[0]
    piece_rows = lax.all_gather(arrived, "tp", axis=1, tiled=True)
    gate_acc = jnp.dot(piece_rows, gate_local, preferred_element_type=jnp.float32)
    up_acc = jnp.dot(piece_rows, up_local, preferred_element_type=jnp.float32)
    hidden = (jax.nn.silu(gate_acc) * up_acc).astype(jnp.bfloat16)
    down_local = down_new[0]
    summed = lax.psum_scatter(
        lax.dot_general(
            down_local, hidden, (((1,), (1,)), ((), ())), preferred_element_type=jnp.float32
        ).astype(jnp.bfloat16),
        "tp",
        scatter_dimension=0,
        tiled=True,
    ).astype(jnp.float32)
    own_columns = summed.shape[0]
    outgoing_back = summed.astype(jnp.bfloat16).reshape(own_columns, fs_count, capacity)
    returned = lax.all_to_all(outgoing_back, "fs", split_axis=1, concat_axis=1, tiled=True).reshape(
        own_columns, experts * capacity
    )
    mixed = lax.dot_general(
        combine,
        returned.astype(jnp.float32),
        (((1,), (1,)), ((), ())),
        precision=lax.Precision.HIGHEST,
        preferred_element_type=jnp.float32,
    )
    return (mixed.astype(jnp.bfloat16), gate_new, up_new, down_new)


MESH = pl.DeviceIdType.MESH
STAGES = 2
ROW_TILE = 256


def flip(index, distance):
    bit = 1
    while bit <= distance:
        if distance & bit:
            index = index + bit - 2 * bit * ((index // bit) % 2)
        bit *= 2
    return index


def rows_of(index, size):
    return pl.ds(pl.multiple_of(index * size, size), size)


def moe_kernel(
    fs,
    tp,
    tokens,
    gain,
    gate,
    up,
    down,
    route,
    route_weight,
    mixed,
    gate_out,
    up_out,
    down_out,
    loaded,
    staged,
    w_gate,
    w_up,
    w_down,
    tok_raw,
    tok_norm,
    hidden,
    pair_own,
    pair_out,
    pair_in,
    z_out,
    z_in,
    back_out,
    back_in,
    load_sem,
    tok_local,
    tf_s,
    tf_r,
    tz_s,
    tz_r,
    tw_s,
    tw_r,
    w_s,
    w_r,
    dn_s,
    dn_r,
    pr_s,
    pr_r,
    z_s,
    z_r,
    bk_s,
    bk_r,
    out_sem,
):
    chips = tp // 2
    f = lax.axis_index("fs")
    t = lax.axis_index("tp")
    z, core = t // 2, t % 2
    sibling = flip(t, 1)
    block, width = tokens.shape
    depth, units = gate.shape[1], gate.shape[2]
    sub = width // STAGES
    total_rows = fs * block
    away = [fs - 1] + list(range(1, fs - 1))
    sources, finals = (gate, up, down), (w_gate, w_up, w_down)

    loads = {}
    for p in range(3):
        for d in away + [0]:
            loads[p, d] = pltpu.make_async_copy(
                sources[p].at[flip(f, d)], loaded.at[p, d], load_sem.at[p, d]
            )
            loads[p, d].start()
    own_tok = pltpu.make_async_copy(tokens, tok_raw.at[t, rows_of(f, block)], tok_local)
    own_tok.start()

    barrier = pltpu.get_barrier_semaphore()
    for d in range(1, fs):
        pl.semaphore_signal(barrier, inc=1, device_id={"fs": flip(f, d)}, device_id_type=MESH)
    for d in range(1, tp):
        pl.semaphore_signal(barrier, inc=1, device_id={"tp": flip(t, d)}, device_id_type=MESH)
    pl.semaphore_wait(barrier, fs + tp - 2)

    sent = []

    def send(src, dst, s_sem, r_sem, **device):
        copy = pltpu.make_async_remote_copy(
            src_ref=src,
            dst_ref=dst,
            send_sem=s_sem,
            recv_sem=r_sem,
            device_id=device,
            device_id_type=MESH,
        )
        copy.start()
        sent.append(copy)
        return copy

    tok_fs = [
        send(tokens, tok_raw.at[t, rows_of(f, block)], tf_s.at[d], tf_r.at[d], fs=flip(f, d))
        for d in range(1, fs)
    ]

    def cast(p, d):
        loads[p, d].wait()
        tile = 64

        @pl.loop(0, depth // tile)
        def _(i):
            rows = rows_of(i, tile)
            value = loaded[p, d, rows, :]
            if p < 2:
                value = value * gain[rows, :]
            value = value.astype(jnp.bfloat16)
            if d:
                staged[p, d - 1, rows, :] = value
            else:
                finals[p][pl.ds(pl.multiple_of(f * depth + i * tile, tile), tile), :] = value

    arrive = {}

    def ship(p, d):
        cast(p, d)
        arrive[p, d] = send(
            staged.at[p, d - 1],
            finals[p].at[rows_of(f, depth)],
            w_s.at[p, d],
            w_r.at[p, d],
            fs=flip(f, d),
        )

    for d in away:
        ship(0, d)

    own_tok.wait()
    for copy in tok_fs:
        copy.wait_recv()
    tok_z = {
        d: send(tok_raw.at[t], tok_raw.at[t], tz_s.at[d], tz_r.at[d], tp=flip(t, 2 * d))
        for d in range(1, chips)
    }
    tok_pair = send(tok_raw.at[t], tok_raw.at[t], tz_s.at[0], tz_r.at[0], tp=sibling)

    for d in away:
        ship(1, d)
    for d in away:
        cast(2, d)
    for u in range(STAGES):
        for d in away:
            for c in range(2):
                arrive[2, u, d, c] = send(
                    staged.at[2, d - 1, pl.ds(c * width + u * sub, sub)],
                    w_down.at[
                        pl.ds(pl.multiple_of(f * depth + (c * width + u * sub), sub), sub)
                    ],
                    dn_s.at[u, d, c],
                    dn_r.at[u, d, c],
                    fs=flip(f, d),
                )
    for p in range(3):
        cast(p, 0)

    forwards = []
    for d in range(1, chips):
        tok_z[d].wait_recv()
        there = flip(t, 2 * d)
        forwards.append(
            send(tok_raw.at[there], tok_raw.at[there], tw_s.at[d], tw_r.at[d], tp=sibling)
        )
    tok_pair.wait_recv()
    for copy in forwards:
        copy.wait_recv()

    @pl.loop(0, total_rows // 64)
    def _(i):
        rows = rows_of(i, 64)
        squares = jnp.zeros((64, 1), jnp.float32)
        for k in range(tp):
            value = tok_raw[k, rows, :].astype(jnp.float32)
            squares = squares + jnp.sum(value * value, axis=1, keepdims=True)
        scale = lax.rsqrt(squares / (width * tp) + epsilon)
        for k in range(tp):
            value = tok_raw[k, rows, :].astype(jnp.float32)
            tok_norm[rows, k * width : (k + 1) * width] = (value * scale).astype(jnp.bfloat16)

    for p in range(2):
        for d in away:
            arrive[p, d].wait_recv()
    outs = [
        pltpu.make_async_copy(w_gate, gate_out, out_sem.at[0]),
        pltpu.make_async_copy(w_up, up_out, out_sem.at[1]),
        pltpu.make_async_copy(w_down, down_out, out_sem.at[2]),
    ]
    outs[0].start()
    outs[1].start()

    @pl.loop(0, total_rows // ROW_TILE)
    def _(i):
        rows = rows_of(i, ROW_TILE)
        value = tok_norm[rows, :]
        gate_acc = jnp.dot(value, w_gate[...], preferred_element_type=jnp.float32)
        up_acc = jnp.dot(value, w_up[...], preferred_element_type=jnp.float32)
        hidden[rows, :] = (jax.nn.silu(gate_acc) * up_acc).astype(jnp.bfloat16)

    def product(u, d):
        s = flip(f, d)
        if d:
            for c in range(2):
                arrive[2, u, d, c].wait_recv()

        def weights(c):
            start = pl.multiple_of(s * depth + c * width + u * sub, sub)
            return w_down[pl.ds(start, sub), :]

        @pl.loop(0, total_rows // ROW_TILE)
        def _(i):
            rows = rows_of(i, ROW_TILE)
            value = hidden[rows, :]
            dims = (((1,), (1,)), ((), ()))
            pair_own[u, d, rows, :] = lax.dot_general(
                value, weights(core), dims, preferred_element_type=jnp.float32
            )
            pair_out[u, d, rows, :] = lax.dot_general(
                value, weights(1 - core), dims, preferred_element_type=jnp.float32
            ).astype(jnp.bfloat16)

        return send(
            pair_out.at[u, d], pair_in.at[u, d], pr_s.at[u, d], pr_r.at[u, d], tp=sibling
        )

    z_sends = []

    def pass_on(u, d, copy):
        s = flip(f, d)
        copy.wait_recv()

        def total(rows):
            value = pair_own[u, d, rows, :] + pair_in[u, d, rows, :].astype(jnp.float32)
            return value.astype(jnp.bfloat16)

        @pl.loop(0, total_rows // ROW_TILE)
        def _(i):
            rows = rows_of(i, ROW_TILE)
            z_out[u, d, rows, :] = total(rows)

        across = pltpu.make_async_remote_copy(
            src_ref=z_out.at[u, d],
            dst_ref=z_in.at[u, z],
            send_sem=z_s.at[u, d],
            recv_sem=z_r.at[u, z],
            device_id={"tp": s * 2 + core},
            device_id_type=MESH,
        )

        @pl.when(s != z)
        def _():
            across.start()

        @pl.when(s == z)
        def _():
            @pl.loop(0, total_rows // ROW_TILE)
            def _(i):
                rows = rows_of(i, ROW_TILE)
                z_in[u, z, rows, :] = z_out[u, d, rows, :]

        z_sends.append((s, across))

    returns = []

    def finish(u):
        for d in range(1, chips):
            there = flip(z, d)
            pltpu.make_async_remote_copy(
                src_ref=z_out.at[u, d],
                dst_ref=z_in.at[u, there],
                send_sem=z_s.at[u, d],
                recv_sem=z_r.at[u, there],
                device_id={"tp": there * 2 + core},
                device_id_type=MESH,
            ).wait_recv()
        for d in away + [0]:
            b = flip(f, d)
            rows = rows_of(b, block)
            value = jnp.zeros((block, sub), jnp.float32)
            for k in range(chips):
                value = value + z_in[u, k, rows, :].astype(jnp.float32)
            value = value.astype(jnp.bfloat16)
            if d:
                back_out[u, d] = value
                returns.append(
                    send(
                        back_out.at[u, d],
                        back_in.at[u, f],
                        bk_s.at[u, d],
                        bk_r.at[u, d],
                        fs=b,
                    )
                )
            else:
                back_in[u, f] = value

    items = [(u, 0) for u in range(STAGES)]
    items += [(u, d) for u in range(STAGES) for d in list(range(1, fs - 1)) + [fs - 1]]
    waiting = None
    for item in items:
        copy = product(*item)
        if waiting is not None:
            pass_on(*waiting)
        waiting = item + (copy,)
    outs[2].start()
    pass_on(*waiting)
    for u in range(STAGES):
        finish(u)
    for copy in returns:
        copy.wait_recv()
    for u in range(STAGES):
        value = jnp.zeros((block, sub), jnp.float32)
        for e in range(fs):
            share = jnp.zeros((block, 1), jnp.float32)
            for k in range(route.shape[1]):
                share = share + jnp.where(
                    route[:, k : k + 1] == e, route_weight[:, k : k + 1], 0.0
                )
            value = value + share * back_in[u, e].astype(jnp.float32)
        mixed[:, u * sub : (u + 1) * sub] = value.astype(jnp.bfloat16)

    for copy in sent:
        copy.wait_send()
    for s, across in z_sends:

        @pl.when(s != z)
        def _():
            across.wait_send()

    for copy in outs:
        copy.wait()


def dense_body(tokens, norm_gain, gate_weight, up_weight, down_weight, route, route_weight):
    fs, tp = lax.axis_size("fs"), lax.axis_size("tp")
    block, width = tokens.shape
    experts, depth, units = gate_weight.shape
    rows, full, sub = fs * block, tp * width, width // STAGES
    whole = pl.BlockSpec(memory_space=pltpu.VMEM)
    far = pl.BlockSpec(memory_space=pl.ANY)
    narrow, dma = jnp.bfloat16, pltpu.SemaphoreType.DMA
    weight = jax.ShapeDtypeStruct((full, units), narrow)
    mixed, gate_new, up_new, down_new = pl.pallas_call(
        functools.partial(moe_kernel, fs, tp),
        out_shape=(jax.ShapeDtypeStruct((block, width), narrow), weight, weight, weight),
        in_specs=[whole, whole, far, far, far, whole, whole],
        out_specs=(whole, far, far, far),
        scratch_shapes=[
            pltpu.VMEM((3, experts, depth, units), jnp.float32),
            pltpu.VMEM((3, fs - 1, depth, units), narrow),
            pltpu.VMEM((full, units), narrow),
            pltpu.VMEM((full, units), narrow),
            pltpu.VMEM((full, units), narrow),
            pltpu.VMEM((tp, rows, width), narrow),
            pltpu.VMEM((rows, full), narrow),
            pltpu.VMEM((rows, units), narrow),
            pltpu.VMEM((STAGES, fs, rows, sub), jnp.float32),
            pltpu.VMEM((STAGES, fs, rows, sub), narrow),
            pltpu.VMEM((STAGES, fs, rows, sub), narrow),
            pltpu.VMEM((STAGES, fs, rows, sub), narrow),
            pltpu.VMEM((STAGES, tp // 2, rows, sub), narrow),
            pltpu.VMEM((STAGES, fs, block, sub), narrow),
            pltpu.VMEM((STAGES, fs, block, sub), narrow),
            dma((3, experts)),
            dma,
            dma((fs,)),
            dma((fs,)),
            dma((tp // 2,)),
            dma((tp // 2,)),
            dma((tp // 2,)),
            dma((tp // 2,)),
            dma((2, fs)),
            dma((2, fs)),
            dma((STAGES, fs, 2)),
            dma((STAGES, fs, 2)),
            dma((STAGES, fs)),
            dma((STAGES, fs)),
            dma((STAGES, fs)),
            dma((STAGES, tp // 2)),
            dma((STAGES, fs)),
            dma((STAGES, fs)),
            dma((3,)),
        ],
        compiler_params=pltpu.CompilerParams(
            collective_id=0, has_side_effects=True, vmem_limit_bytes=64000 * 1024
        ),
    )(tokens, norm_gain[:, None], gate_weight, up_weight, down_weight, route, route_weight)
    return mixed, gate_new[None], up_new[None], down_new[None]


def body(tokens, norm_gain, gate_weight, up_weight, down_weight, route, route_weight):
    fs, tp = lax.axis_size("fs"), lax.axis_size("tp")
    fits = (
        fs == 4
        and tp == 2 * fs
        and gate_weight.shape[0] == fs
        and tokens.shape[1] % (128 * STAGES) == 0
        and tokens.shape[0] % 64 == 0
        and gate_weight.shape[1] == 2 * tokens.shape[1]
        and tokens.shape[0] * fs * tokens.shape[1] * tp <= 1024 * 2048
    )
    chosen = dense_body if fits else slotted_body
    return chosen(tokens, norm_gain, gate_weight, up_weight, down_weight, route, route_weight)


def solution(mesh):
    in_specs = (
        P("fs", "tp"),
        P("fs"),
        P(None, "fs", "tp"),
        P(None, "fs", "tp"),
        P(None, "fs", "tp"),
        P("fs", None),
        P("fs", None),
    )
    out_specs = (P("fs", "tp"), P("fs", None, "tp"), P("fs", None, "tp"), P("fs", None, "tp"))
    return jax.shard_map(body, mesh=mesh, in_specs=in_specs, out_specs=out_specs, check_vma=False)
```

```python
import functools

import jax
import jax.numpy as jnp
from jax import lax
from jax.experimental import pallas as pl
from jax.experimental.pallas import tpu as pltpu
from jax.sharding import PartitionSpec as P

epsilon = 1e-05


def slot_table(route, block_rows, expert_count):
    pair_ids = route.reshape(-1, block_rows * route.shape[1])
    onehot = (
        pair_ids[:, :, None] == jnp.arange(expert_count, dtype=jnp.int32)[None, None, :]
    ).astype(jnp.int32)
    before = jnp.cumsum(onehot, axis=1) - onehot
    return jnp.sum(before * onehot, axis=2).reshape(route.shape)


def slotted_body(tokens, norm_gain, gate_weight, up_weight, down_weight, route, route_weight):
    experts = gate_weight.shape[0]
    tok_rows = tokens.shape[0]
    columns = tokens.shape[1]
    fs_count = lax.axis_size("fs")
    capacity = 4 * tok_rows // fs_count
    gain_col = norm_gain[None, :, None]
    gate_cast = (gate_weight * gain_col).astype(jnp.bfloat16)
    up_cast = (up_weight * gain_col).astype(jnp.bfloat16)
    down_cast = down_weight.astype(jnp.bfloat16)
    gate_new, up_new, down_new = (
        lax.all_to_all(gate_cast, "fs", split_axis=0, concat_axis=1, tiled=True),
        lax.all_to_all(up_cast, "fs", split_axis=0, concat_axis=1, tiled=True),
        lax.all_to_all(down_cast, "fs", split_axis=0, concat_axis=1, tiled=True),
    )
    slot_of = slot_table(route, tok_rows, experts)
    target = route * capacity + slot_of
    slot_lanes = jnp.arange(experts * capacity, dtype=jnp.int32)
    slot_hits = target[:, :, None] == slot_lanes[None, None, :]
    token_iota = jnp.arange(tok_rows, dtype=jnp.int32)[:, None, None]
    lane_token = jnp.sum(jnp.where(slot_hits, token_iota + 1, 0), axis=(0, 1)) - 1
    lane_token = jnp.where(lane_token < 0, tok_rows, lane_token)
    combine = jnp.sum(jnp.where(slot_hits, route_weight[:, :, None], 0.0), axis=1)
    tok_float = tokens.astype(jnp.float32)
    square_sum = lax.psum(jnp.sum(tok_float * tok_float, axis=1), "tp")
    full_width = columns * lax.axis_size("tp")
    normed = (tok_float * lax.rsqrt(square_sum / full_width + epsilon)[:, None]).astype(
        jnp.bfloat16
    )
    padded = jnp.concatenate([normed, jnp.zeros((1, columns), jnp.bfloat16)], axis=0)
    outgoing = padded[lane_token].reshape(experts, capacity, columns)
    arrived = lax.all_to_all(outgoing, "fs", split_axis=0, concat_axis=0, tiled=True).reshape(
        -1, columns
    )
    gate_local = gate_new[0]
    up_local = up_new[0]
    piece_rows = lax.all_gather(arrived, "tp", axis=1, tiled=True)
    gate_acc = jnp.dot(piece_rows, gate_local, preferred_element_type=jnp.float32)
    up_acc = jnp.dot(piece_rows, up_local, preferred_element_type=jnp.float32)
    hidden = (jax.nn.silu(gate_acc) * up_acc).astype(jnp.bfloat16)
    down_local = down_new[0]
    summed = lax.psum_scatter(
        lax.dot_general(
            down_local, hidden, (((1,), (1,)), ((), ())), preferred_element_type=jnp.float32
        ).astype(jnp.bfloat16),
        "tp",
        scatter_dimension=0,
        tiled=True,
    ).astype(jnp.float32)
    own_columns = summed.shape[0]
    outgoing_back = summed.astype(jnp.bfloat16).reshape(own_columns, fs_count, capacity)
    returned = lax.all_to_all(outgoing_back, "fs", split_axis=1, concat_axis=1, tiled=True).reshape(
        own_columns, experts * capacity
    )
    mixed = lax.dot_general(
        combine,
        returned.astype(jnp.float32),
        (((1,), (1,)), ((), ())),
        precision=lax.Precision.HIGHEST,
        preferred_element_type=jnp.float32,
    )
    return (mixed.astype(jnp.bfloat16), gate_new, up_new, down_new)


MESH = pl.DeviceIdType.MESH
STAGES = 2
ROW_TILE = 256


def flip(index, distance):
    bit = 1
    while bit <= distance:
        if distance & bit:
            index = index + bit - 2 * bit * ((index // bit) % 2)
        bit *= 2
    return index


def rows_of(index, size):
    return pl.ds(pl.multiple_of(index * size, size), size)


def moe_kernel(
    fs,
    tp,
    tokens,
    gain,
    gate,
    up,
    down,
    route,
    route_weight,
    mixed,
    gate_out,
    up_out,
    down_out,
    loaded,
    staged,
    w_gate,
    w_up,
    w_down,
    tok_raw,
    tok_norm,
    hidden,
    pair_own,
    pair_out,
    pair_in,
    z_out,
    z_in,
    back_out,
    back_in,
    gain_col,
    load_sem,
    tok_local,
    tf_s,
    tf_r,
    tz_s,
    tz_r,
    tw_s,
    tw_r,
    w_s,
    w_r,
    dn_s,
    dn_r,
    pr_s,
    pr_r,
    z_s,
    z_r,
    bk_s,
    bk_r,
    out_sem,
):
    chips = tp // 2
    f = lax.axis_index("fs")
    t = lax.axis_index("tp")
    z, core = t // 2, t % 2
    sibling = flip(t, 1)
    block, width = tokens.shape
    depth, units = gate.shape[1], gate.shape[2]
    sub = width // STAGES
    total_rows = fs * block
    away = [fs - 1] + list(range(1, fs - 1))
    sources, finals = (gate, up, down), (w_gate, w_up, w_down)

    barrier = pltpu.get_barrier_semaphore()
    for d in range(1, fs):
        pl.semaphore_signal(barrier, inc=1, device_id={"fs": flip(f, d)}, device_id_type=MESH)
    for d in range(1, tp):
        pl.semaphore_signal(barrier, inc=1, device_id={"tp": flip(t, d)}, device_id_type=MESH)
    loads = {}
    for p in range(3):
        for d in away + [0]:
            loads[p, d] = pltpu.make_async_copy(
                sources[p].at[flip(f, d)], loaded.at[p, d], load_sem.at[p, d]
            )
            loads[p, d].start()
    own_tok = pltpu.make_async_copy(tokens, tok_raw.at[t, rows_of(f, block)], tok_local)
    own_tok.start()

    gain_col[...] = jnp.broadcast_to(gain[...], (128, depth)).T
    pl.semaphore_wait(barrier, fs + tp - 2)

    sent = []

    def send(src, dst, s_sem, r_sem, **device):
        copy = pltpu.make_async_remote_copy(
            src_ref=src,
            dst_ref=dst,
            send_sem=s_sem,
            recv_sem=r_sem,
            device_id=device,
            device_id_type=MESH,
        )
        copy.start()
        sent.append(copy)
        return copy

    tok_fs = [
        send(tokens, tok_raw.at[t, rows_of(f, block)], tf_s.at[d], tf_r.at[d], fs=flip(f, d))
        for d in away
    ]

    def cast(p, d):
        loads[p, d].wait()
        tile = 64

        @pl.loop(0, depth // tile)
        def _(i):
            rows = rows_of(i, tile)
            value = loaded[p, d, rows, :]
            if p < 2:
                value = value * gain_col[rows, 0:1]
            value = value.astype(jnp.bfloat16)
            if d:
                staged[p, d - 1, rows, :] = value
            else:
                finals[p][pl.ds(pl.multiple_of(f * depth + i * tile, tile), tile), :] = value

    arrive = {}

    def ship(p, d):
        cast(p, d)
        arrive[p, d] = send(
            staged.at[p, d - 1],
            finals[p].at[rows_of(f, depth)],
            w_s.at[p, d],
            w_r.at[p, d],
            fs=flip(f, d),
        )

    for d in away:
        ship(0, d)

    own_tok.wait()
    for copy in tok_fs:
        copy.wait_recv()
    tok_z = {
        d: send(tok_raw.at[t], tok_raw.at[t], tz_s.at[d], tz_r.at[d], tp=flip(t, 2 * d))
        for d in range(1, chips)
    }
    tok_pair = send(tok_raw.at[t], tok_raw.at[t], tz_s.at[0], tz_r.at[0], tp=sibling)

    for d in away:
        ship(1, d)
    for d in away:
        cast(2, d)
    for u in range(STAGES):
        for d in away:
            for c in range(2):
                arrive[2, u, d, c] = send(
                    staged.at[2, d - 1, pl.ds(c * width + u * sub, sub)],
                    w_down.at[
                        pl.ds(pl.multiple_of(f * depth + (c * width + u * sub), sub), sub)
                    ],
                    dn_s.at[u, d, c],
                    dn_r.at[u, d, c],
                    fs=flip(f, d),
                )
    for p in range(3):
        cast(p, 0)

    forwards = []
    for d in range(1, chips):
        tok_z[d].wait_recv()
        there = flip(t, 2 * d)
        forwards.append(
            send(tok_raw.at[there], tok_raw.at[there], tw_s.at[d], tw_r.at[d], tp=sibling)
        )
    tok_pair.wait_recv()
    for copy in forwards:
        copy.wait_recv()

    @pl.loop(0, total_rows // 64)
    def _(i):
        rows = rows_of(i, 64)
        squares = jnp.zeros((64, 1), jnp.float32)
        for k in range(tp):
            value = tok_raw[k, rows, :].astype(jnp.float32)
            squares = squares + jnp.sum(value * value, axis=1, keepdims=True)
        scale = lax.rsqrt(squares / (width * tp) + epsilon)
        for k in range(tp):
            value = tok_raw[k, rows, :].astype(jnp.float32)
            tok_norm[rows, k * width : (k + 1) * width] = (value * scale).astype(jnp.bfloat16)

    for p in range(2):
        for d in away:
            arrive[p, d].wait_recv()
    outs = [
        pltpu.make_async_copy(w_gate, gate_out, out_sem.at[0]),
        pltpu.make_async_copy(w_up, up_out, out_sem.at[1]),
        pltpu.make_async_copy(w_down, down_out, out_sem.at[2]),
    ]
    outs[0].start()
    outs[1].start()

    @pl.loop(0, total_rows // ROW_TILE)
    def _(i):
        rows = rows_of(i, ROW_TILE)
        value = tok_norm[rows, :]
        gate_acc = jnp.dot(value, w_gate[...], preferred_element_type=jnp.float32)
        up_acc = jnp.dot(value, w_up[...], preferred_element_type=jnp.float32)
        hidden[rows, :] = (jax.nn.silu(gate_acc) * up_acc).astype(jnp.bfloat16)

    def product(u, d):
        s = flip(f, d)
        if d:
            for c in range(2):
                arrive[2, u, d, c].wait_recv()

        def weights(c):
            start = pl.multiple_of(s * depth + c * width + u * sub, sub)
            return w_down[pl.ds(start, sub), :]

        @pl.loop(0, total_rows // ROW_TILE)
        def _(i):
            rows = rows_of(i, ROW_TILE)
            value = hidden[rows, :]
            dims = (((1,), (1,)), ((), ()))
            pair_own[u, d, rows, :] = lax.dot_general(
                value, weights(core), dims, preferred_element_type=jnp.float32
            )
            pair_out[u, d, rows, :] = lax.dot_general(
                value, weights(1 - core), dims, preferred_element_type=jnp.float32
            ).astype(jnp.bfloat16)

        return send(
            pair_out.at[u, d], pair_in.at[u, d], pr_s.at[u, d], pr_r.at[u, d], tp=sibling
        )

    z_sends = []

    def pass_on(u, d, copy):
        s = flip(f, d)
        copy.wait_recv()

        def total(rows):
            value = pair_own[u, d, rows, :] + pair_in[u, d, rows, :].astype(jnp.float32)
            return value.astype(jnp.bfloat16)

        @pl.loop(0, total_rows // ROW_TILE)
        def _(i):
            rows = rows_of(i, ROW_TILE)
            z_out[u, d, rows, :] = total(rows)

        across = pltpu.make_async_remote_copy(
            src_ref=z_out.at[u, d],
            dst_ref=z_in.at[u, z],
            send_sem=z_s.at[u, d],
            recv_sem=z_r.at[u, z],
            device_id={"tp": s * 2 + core},
            device_id_type=MESH,
        )

        @pl.when(s != z)
        def _():
            across.start()

        @pl.when(s == z)
        def _():
            @pl.loop(0, total_rows // ROW_TILE)
            def _(i):
                rows = rows_of(i, ROW_TILE)
                z_in[u, z, rows, :] = z_out[u, d, rows, :]

        z_sends.append((s, across))

    returns = []

    def finish(u):
        for d in range(1, chips):
            there = flip(z, d)
            pltpu.make_async_remote_copy(
                src_ref=z_out.at[u, d],
                dst_ref=z_in.at[u, there],
                send_sem=z_s.at[u, d],
                recv_sem=z_r.at[u, there],
                device_id={"tp": there * 2 + core},
                device_id_type=MESH,
            ).wait_recv()
        for d in away + [0]:
            b = flip(f, d)
            rows = rows_of(b, block)
            value = jnp.zeros((block, sub), jnp.float32)
            for k in range(chips):
                value = value + z_in[u, k, rows, :].astype(jnp.float32)
            value = value.astype(jnp.bfloat16)
            if d:
                back_out[u, d] = value
                returns.append(
                    send(
                        back_out.at[u, d],
                        back_in.at[u, f],
                        bk_s.at[u, d],
                        bk_r.at[u, d],
                        fs=b,
                    )
                )
            else:
                back_in[u, f] = value

    items = [(u, 0) for u in range(STAGES)]
    items += [(u, d) for u in range(STAGES) for d in list(range(1, fs - 1)) + [fs - 1]]
    waiting = None
    for item in items:
        copy = product(*item)
        if waiting is not None:
            pass_on(*waiting)
        waiting = item + (copy,)
    outs[2].start()
    pass_on(*waiting)
    for u in range(STAGES):
        finish(u)
    for copy in returns:
        copy.wait_recv()
    for u in range(STAGES):
        value = jnp.zeros((block, sub), jnp.float32)
        for e in range(fs):
            share = jnp.zeros((1, block), jnp.float32)
            for k in range(route.shape[0]):
                share = share + jnp.where(
                    route[k : k + 1, :] == e, route_weight[k : k + 1, :], 0.0
                )
            share = jnp.broadcast_to(share, (sub, block)).T
            value = value + share * back_in[u, e].astype(jnp.float32)
        mixed[:, u * sub : (u + 1) * sub] = value.astype(jnp.bfloat16)

    for copy in sent:
        copy.wait_send()
    for s, across in z_sends:

        @pl.when(s != z)
        def _():
            across.wait_send()

    for copy in outs:
        copy.wait()


def dense_body(tokens, norm_gain, gate_weight, up_weight, down_weight, route, route_weight):
    fs, tp = lax.axis_size("fs"), lax.axis_size("tp")
    block, width = tokens.shape
    experts, depth, units = gate_weight.shape
    rows, full, sub = fs * block, tp * width, width // STAGES
    whole = pl.BlockSpec(memory_space=pltpu.VMEM)
    far = pl.BlockSpec(memory_space=pl.ANY)
    narrow, dma = jnp.bfloat16, pltpu.SemaphoreType.DMA
    weight = jax.ShapeDtypeStruct((full, units), narrow)
    mixed, gate_new, up_new, down_new = pl.pallas_call(
        functools.partial(moe_kernel, fs, tp),
        out_shape=(jax.ShapeDtypeStruct((block, width), narrow), weight, weight, weight),
        in_specs=[whole, whole, far, far, far, whole, whole],
        out_specs=(whole, far, far, far),
        scratch_shapes=[
            pltpu.VMEM((3, experts, depth, units), jnp.float32),
            pltpu.VMEM((3, fs - 1, depth, units), narrow),
            pltpu.VMEM((full, units), narrow),
            pltpu.VMEM((full, units), narrow),
            pltpu.VMEM((full, units), narrow),
            pltpu.VMEM((tp, rows, width), narrow),
            pltpu.VMEM((rows, full), narrow),
            pltpu.VMEM((rows, units), narrow),
            pltpu.VMEM((STAGES, fs, rows, sub), jnp.float32),
            pltpu.VMEM((STAGES, fs, rows, sub), narrow),
            pltpu.VMEM((STAGES, fs, rows, sub), narrow),
            pltpu.VMEM((STAGES, fs, rows, sub), narrow),
            pltpu.VMEM((STAGES, tp // 2, rows, sub), narrow),
            pltpu.VMEM((STAGES, fs, block, sub), narrow),
            pltpu.VMEM((STAGES, fs, block, sub), narrow),
            pltpu.VMEM((depth, 128), jnp.float32),
            dma((3, experts)),
            dma,
            dma((fs,)),
            dma((fs,)),
            dma((tp // 2,)),
            dma((tp // 2,)),
            dma((tp // 2,)),
            dma((tp // 2,)),
            dma((2, fs)),
            dma((2, fs)),
            dma((STAGES, fs, 2)),
            dma((STAGES, fs, 2)),
            dma((STAGES, fs)),
            dma((STAGES, fs)),
            dma((STAGES, fs)),
            dma((STAGES, tp // 2)),
            dma((STAGES, fs)),
            dma((STAGES, fs)),
            dma((3,)),
        ],
        compiler_params=pltpu.CompilerParams(
            collective_id=0, has_side_effects=True, vmem_limit_bytes=64000 * 1024
        ),
    )(tokens, norm_gain[None, :], gate_weight, up_weight, down_weight, route.T, route_weight.T)
    return mixed, gate_new[None], up_new[None], down_new[None]


def body(tokens, norm_gain, gate_weight, up_weight, down_weight, route, route_weight):
    fs, tp = lax.axis_size("fs"), lax.axis_size("tp")
    fits = (
        fs == 4
        and tp == 2 * fs
        and gate_weight.shape[0] == fs
        and tokens.shape[1] % (128 * STAGES) == 0
        and tokens.shape[0] % 64 == 0
        and gate_weight.shape[1] == 2 * tokens.shape[1]
        and tokens.shape[0] * fs * tokens.shape[1] * tp <= 1024 * 2048
    )
    chosen = dense_body if fits else slotted_body
    return chosen(tokens, norm_gain, gate_weight, up_weight, down_weight, route, route_weight)


def solution(mesh):
    in_specs = (
        P("fs", "tp"),
        P("fs"),
        P(None, "fs", "tp"),
        P(None, "fs", "tp"),
        P(None, "fs", "tp"),
        P("fs", None),
        P("fs", None),
    )
    out_specs = (P("fs", "tp"), P("fs", None, "tp"), P("fs", None, "tp"), P("fs", None, "tp"))
    return jax.shard_map(body, mesh=mesh, in_specs=in_specs, out_specs=out_specs, check_vma=False)
```
